32 devices in a mesh: grp: 2 (over y), fs: 4 (over z), tp: 4 (over x, core).
Axes of the slice: x: 2, y: 2, z: 4, core: 2. Of those that a mesh axis runs over, the one named last changes fastest.
Arguments:
- tokens: bfloat16 [4096, 2048], P(('grp', 'fs')), parts along dimension 0, may hold values from -6 to 6
- pre_gain: float32 [2048], replicated, may hold values from 0.1 to 1.9
- up_weight: float32 [2048, 8192], P('fs', 'tp'), may hold values from -0.125 to 0.125
- up_scale: float32 [8192], P('tp'), may hold values from 0.3 to 3
- down_weight: float32 [8192, 2048], P('tp', 'fs'), may hold values from -0.0625 to 0.0625
- down_scale: float32 [2048], P('fs'), may hold values from 0.3 to 3
- post_gain: float32 [2048], replicated, may hold values from 0.1 to 1.9
Outputs:
- mixed: bfloat16 [4096, 2048], P(('grp', 'fs')), parts along dimension 0
The draws below stay inside these ranges and needn't reach their ends.
There are 2 independent parts, one for each index of `grp`. The reference program is written for one: setup_inputs(seed, part) draws one part's arguments, and reference() takes and returns one part's arrays. A program takes and returns all parts, laid end to end along the dimension named above; an argument that names none is the same for every part. Nothing has to cross between parts.
All inputs are finite; a program needn't handle non-finite values.
Results may differ from the reference program's by a relative error of at most 0.01.
Values may be sent and summed in bfloat16 or wider, within the bound.
A program may use at most 64 MiB of HBM per device.

```python
import math
import jax
import jax.numpy as jnp
from jax import lax

D = 2048
FF = 8192
TOK_DEV = 512
TOKENS = 2048
N_FS = 4
N_TP = 4


def levels(rng, shape, cuts, least, top_value):
    def one(dim, blocks):
        steps = jax.random.uniform(jax.random.fold_in(jax.random.fold_in(rng, 6), dim), (blocks,), jnp.float32, least / len(cuts), top_value / len(cuts))
        return jnp.repeat(jnp.exp(steps), shape[dim] // blocks).reshape((-1,) + (1,) * (len(shape) - dim - 1))

    gain = one(*cuts[0])
    for cut in cuts[1:]:
        gain = gain * one(*cut)
    return gain


def scatter_about(key, shape, scale, limit, split=(), dtype=jnp.bfloat16):
    gain = levels(key, shape, split, -0.22, 0.18) if split else 1.0
    values = jax.random.normal(key, shape, jnp.float32) * scale * gain
    return jnp.minimum(jnp.maximum(values, -limit), limit).astype(dtype)


def setup_inputs(seed: int = 0, part: int = 0) -> dict:
    seeds = jax.random.split(jax.random.key(seed), 8)
    part_keys = jax.random.split(jax.random.fold_in(seeds[7], part), 8)
    tokens = scatter_about(part_keys[0], (TOKENS, D), 1.0, 6.0, ((0, 4),))
    pre_gain = jnp.clip(1.0 + 0.18 * jax.random.normal(seeds[1], (D,), jnp.float32), 0.1, 1.9)
    up_weight = scatter_about(seeds[2], (D, FF), D ** -0.5, 0.125, ((0, 4), (1, 4)), jnp.float32)
    up_scale = jnp.clip(jnp.exp(math.log(3.0) - 2.3025851 * jax.random.uniform(seeds[3], (FF,), jnp.float32) ** levels(seeds[3], (FF,), ((0, 4),), -0.2, 0.2)), 0.3, 3.0)
    down_weight = scatter_about(seeds[4], (FF, D), FF ** -0.5, 0.0625, ((0, 4), (1, 4)), jnp.float32)
    down_scale = jnp.clip(jnp.exp(math.log(3.0) - 2.3025851 * jax.random.uniform(seeds[5], (D,), jnp.float32) ** levels(seeds[5], (D,), ((0, 4),), -0.2, 0.2)), 0.3, 3.0)
    post_gain = jnp.clip(1.0 + 0.18 * jax.random.normal(seeds[6], (D,), jnp.float32), 0.1, 1.9)
    return {"tokens": tokens, "pre_gain": pre_gain, "up_weight": up_weight, "up_scale": up_scale, "down_weight": down_weight, "down_scale": down_scale, "post_gain": post_gain}


epsilon = 1e-06

def rms_rows(values, scaling):
    return values * lax.rsqrt(lax.optimization_barrier(jnp.mean(values * values, axis=-1, keepdims=True)) + epsilon) * scaling

def reference(tokens, pre_gain, up_weight, up_scale, down_weight, down_scale, post_gain):
    up_cast = up_weight.astype(jnp.bfloat16)
    down_cast = down_weight.astype(jnp.bfloat16)
    block_width = FF // N_TP

    def row_block(rows):
        residual = rows.astype(jnp.float32)
        normed = rms_rows(residual, pre_gain).astype(jnp.bfloat16)
        lifted = jnp.dot(normed, up_cast, preferred_element_type=jnp.float32) * up_scale
        hidden = jnp.square(jax.nn.relu(lifted)).astype(jnp.bfloat16)
        running = jnp.zeros((rows.shape[0], D), jnp.float32)
        for member in range(N_TP):
            low = member * block_width
            high = low + block_width
            partial_value = jnp.dot(hidden[:, low:high], down_cast[low:high], preferred_element_type=jnp.float32) * down_scale
            partial_value = lax.optimization_barrier(partial_value.astype(jnp.bfloat16))
            running = running + partial_value.astype(jnp.float32)
        branch = lax.optimization_barrier(running.astype(jnp.bfloat16)).astype(jnp.float32)
        return (residual + rms_rows(branch, post_gain)).astype(jnp.bfloat16)
    result = lax.map(row_block, tokens.reshape(N_FS, TOK_DEV, D))
    return result.reshape(N_FS * TOK_DEV, D)
```

```python
import functools

import jax
import jax.numpy as jnp
from jax import lax
from jax.experimental import pallas as pl
from jax.experimental.pallas import tpu as pltpu
from jax.sharding import PartitionSpec as P

epsilon = 1e-06
MESH = pl.DeviceIdType.MESH
PIECES = 4
WIDTHS = ((2, 2), (2, 2), (2, 2), (2, 1, 1))


def rms_rows(values, scaling):
    return values * lax.rsqrt(jnp.mean(values * values, axis=-1, keepdims=True) + epsilon) * scaling


def activate(lifted, up_scale):
    return jnp.square(jax.nn.relu(lifted * up_scale)).astype(jnp.bfloat16)


def plain(tokens, pre_gain, up_weight, up_scale, down_weight, down_scale, post_gain):
    residual = tokens.astype(jnp.float32)
    normed = rms_rows(residual, pre_gain).astype(jnp.bfloat16)
    up_cast = up_weight.astype(jnp.bfloat16)
    down_cast = down_weight.astype(jnp.bfloat16)
    column_scales = lax.all_gather(down_scale, "fs", axis=0, tiled=True)
    up_full, down_full = (
        lax.all_gather(up_cast, "fs", axis=0, tiled=True),
        lax.all_gather(down_cast, "fs", axis=1, tiled=True),
    )
    lifted = jnp.dot(normed, up_full, preferred_element_type=jnp.float32)
    hidden = activate(lifted, up_scale)
    partials = jnp.dot(hidden, down_full, preferred_element_type=jnp.float32)
    partials = (partials * column_scales).astype(jnp.bfloat16)
    summed = lax.psum(partials, "tp").astype(jnp.float32)
    branch = lax.optimization_barrier(summed.astype(jnp.bfloat16)).astype(jnp.float32)
    return (residual + rms_rows(branch, post_gain)).astype(jnp.bfloat16)


def kernel(tokens, up_in, down_in, up_scale, down_scale, pre_gain, post_gain, out, res, up_f32, down_f32, up, down,
           tok, acc, hid, scl, keep, core_out, core_in, y_out, y_in, xz_out, x_in, branch, send, up_recv, down_recv,
           tok_recv, scl_recv, core_recv, y_recv, x_recv, br_recv, local, one_sem, out_sem):
    g, z, t = lax.axis_index("grp"), lax.axis_index("fs"), lax.axis_index("tp")
    core, x = lax.rem(t, 2), t // 2
    pair = z // 2
    outer, inner, other = 3 * pair, 1 + pair, 2 - pair
    outer2 = 3 - outer
    is_outer = z == outer
    n_tp, np_ = 4, PIECES
    rows, width = tokens.shape
    depth, half = up_in.shape[0], up_in.shape[1] // 2
    du, dc, quarter = depth // np_, depth // np_, rows // np_
    core_peer, x_peer, cross_peer = x * 2 + 1 - core, (1 - x) * 2 + core, (1 - x) * 2 + 1 - core
    bf, f32 = jnp.bfloat16, jnp.float32

    def at(i, size):
        return pl.ds(pl.multiple_of(i * size, size), size)

    def load(kind, c):
        if kind == 0:
            copy = up_in.at[pl.ds(c * du, du), at(g, half)], up_f32.at[pl.ds(c * du, du), :]
        else:
            copy = down_in.at[at(g, half), pl.ds(c * dc, dc)], down_f32.at[:, pl.ds(c * dc, dc)]
        return pltpu.make_async_copy(*copy, local.at[kind, c])

    load(0, 0).start()
    fetch = pltpu.make_async_copy(tokens, res, one_sem.at[0])
    fetch.start()
    for c in range(1, np_):
        load(0, c).start()
    for c in range(np_):
        load(1, c).start()

    barrier = pltpu.get_barrier_semaphore()
    peers = [{"fs": lax.rem(z + o, 4)} for o in range(1, 4)] + [{"grp": 1 - g}]
    peers += [{"tp": lax.rem(t + o, n_tp)} for o in range(1, n_tp)]
    for peer in peers:
        pl.semaphore_signal(barrier, inc=1, device_id=peer, device_id_type=MESH)
    pl.semaphore_wait(barrier, len(peers))

    def remote(src, dst, s, r, peer):
        return pltpu.make_async_remote_copy(src_ref=src, dst_ref=dst, send_sem=send.at[s], recv_sem=r,
                                            device_id=peer, device_id_type=MESH)

    def same(ref, s, r, peer):
        return remote(ref, ref, s, r, peer)

    def slot(kind, zz, c):
        if kind == 0:
            return up.at[at(zz * np_ + c, du), :], up_recv.at[zz, c]
        return down.at[zz * np_ + c], down_recv.at[zz, c]

    def cast(kind, c):
        load(kind, c).wait()
        if kind == 0:
            up[at(z * np_ + c, du), :] = up_f32[pl.ds(c * du, du), :].astype(bf)
        else:
            down[z * np_ + c] = down_f32[:, pl.ds(c * dc, dc)].astype(bf)

    def weight(kind, zz, c, s, peer):
        ref, r = slot(kind, zz, c)
        return same(ref, s, r, peer)

    def arrived(kind, zz, c):
        weight(kind, zz, c, 0, {"fs": other}).wait_recv()

    def piece(gg, kind, k):
        b = kind * 2 + gg
        return tok.at[at(b * np_ + k, quarter), :], tok_recv.at[b, k]

    def pass_tok(gg, kind, k, s, peer):
        ref, r = piece(gg, kind, k)
        return same(ref, s, r, peer)

    def have_tok(gg, kind, k):
        pass_tok(gg, kind, k, 0, {"fs": other}).wait_recv()

    def norm(b, k):
        def one(i, _):
            source = pl.ds(pl.multiple_of(k * quarter + i * 64, 64), 64)
            target = pl.ds(pl.multiple_of((b * np_ + k) * quarter + i * 64, 64), 64)
            tok[target, :] = rms_rows(res[source, :].astype(f32), pre_gain[...]).astype(bf)
            return 0
        lax.fori_loop(0, quarter // 64, one, 0)

    blocks = (inner, outer, other, outer2)
    units = []
    for j, widths in enumerate(WIDTHS):
        k = 0
        for w in widths:
            units.append((blocks[j], k, w, j))
            k += w
    n = len(units)

    def part(ref, i):
        zz, k, w, _ = units[i]
        return ref.at[pl.ds(zz * np_ + k, w)]

    started = []
    counter = [0]

    def fresh():
        counter[0] += 1
        return counter[0] - 1

    def go(copy):
        copy.start()
        started.append(copy)

    last = [fresh() for _ in range(n)]

    def value(i, first, second):
        zz, k, w, _ = units[i]
        for j in range(w):
            b = zz * np_ + k + j
            total = first[b].astype(f32) + second[b].astype(f32)
            branch[b] = (total * scl[zz, :, pl.ds((k + j) * dc, dc)]).astype(bf)

    def share(i):
        return same(part(branch, i), last[i], br_recv.at[i], {"tp": core_peer})

    for o in range(1, 4):
        go(remote(down_scale, scl.at[z], fresh(), scl_recv.at[z], {"fs": lax.rem(z + o, 4)}))
    own_scale = pltpu.make_async_copy(down_scale, scl.at[z], one_sem.at[1])
    own_scale.start()

    def scales():
        own_scale.wait()
        for o in range(1, 4):
            zz = lax.rem(z + o, 4)
            remote(down_scale, scl.at[zz], 0, scl_recv.at[zz], {"fs": zz}).wait_recv()

    @pl.when(is_outer)
    def _():
        mark = len(started)
        to = {"fs": inner}
        fetch.wait()
        norm(2 + g, t)
        go(pass_tok(g, 1, t, fresh(), to))
        for kind in range(2):
            for c in range(np_):
                cast(kind, c)
                go(weight(kind, z, c, fresh(), to))
        scales()

        @pl.when(core == 1)
        def _():
            relays = [fresh() for _ in range(n)]

            def relay(i):
                return remote(part(x_in, i), part(y_in, i), relays[i], y_recv.at[i], {"tp": x_peer})

            for i in range(n + 1):
                if i < n:
                    remote(part(x_in, i), part(x_in, i), 0, x_recv.at[i], {"fs": inner}).wait_recv()
                    relay(i).start()
                if i >= 1:
                    relay(i - 1).wait_recv()
                    value(i - 1, x_in, y_in)
                    share(i - 1).start()
            for i in range(n):
                relay(i).wait_send()
                share(i).wait_send()

        @pl.when(core == 0)
        def _():
            for i in range(n):
                share(i).wait_recv()

        for copy in started[mark:]:
            copy.wait_send()
        del started[mark:]

    @pl.when(jnp.logical_not(is_outer))
    def _():
        mark = len(started)
        across, beside, next_core = {"fs": other}, {"grp": 1 - g}, {"tp": core_peer}
        for c in range(np_):
            cast(0, c)
            go(weight(0, z, c, fresh(), across))
        fetch.wait()
        for j in range(np_):
            k = lax.rem(core * 2 + j, 4)
            norm(g, k)
            if j < 2:
                go(pass_tok(g, 0, k, fresh(), beside))
        for c in range(np_):
            cast(1, c)

        have_tok(g, 1, t)
        go(pass_tok(g, 1, t, fresh(), {"tp": x_peer}))
        go(pass_tok(g, 1, t, fresh(), beside))
        go(pass_tok(g, 1, t, fresh(), next_core))
        go(pass_tok(g, 1, t, fresh(), {"tp": cross_peer}))

        def forward(kind, c):
            arrived(kind, outer, c)
            go(weight(kind, outer, c, fresh(), across))

        def hand_on(kind, k):
            have_tok(1 - g, kind, k)
            go(pass_tok(1 - g, kind, k, fresh(), next_core))

        forward(0, 0)
        hand_on(0, core * 2)
        forward(0, 1)
        hand_on(0, core * 2 + 1)
        have_tok(g, 1, x_peer)
        go(pass_tok(g, 1, x_peer, fresh(), beside))
        forward(0, 2)
        forward(0, 3)
        for c in range(np_):
            go(weight(1, z, c, fresh(), across))

        tile = 256
        most = 3 * depth
        low, rest = pair * depth, outer2 * depth
        most_at = pl.ds(pl.multiple_of(low, depth), most)
        rest_at = pl.ds(pl.multiple_of(rest, depth), depth)

        def lift_most(b):
            lines = at(b, rows)

            def one(i, _):
                columns = at(i, tile)
                acc[lines, columns] = jnp.dot(tok[lines, most_at], up[most_at, columns], preferred_element_type=f32)
                return 0
            lax.fori_loop(0, half // tile, one, 0)

        def lift_rest(b):
            lines = at(b, rows)

            def one(i, _):
                columns = at(i, tile)
                lifted = acc[lines, columns] + jnp.dot(tok[lines, rest_at], up[rest_at, columns],
                                                       preferred_element_type=f32)
                whole = pl.ds(pl.multiple_of(g * half + i * tile, tile), tile)
                hid[lines, columns] = activate(lifted, up_scale[:, whole])
                return 0
            lax.fori_loop(0, half // tile, one, 0)

        for c in range(np_):
            arrived(0, other, c)
        lift_most(g)
        have_tok(g, 1, core_peer)
        have_tok(g, 1, cross_peer)
        lift_most(2 + g)
        hand_on(1, t)
        have_tok(1 - g, 0, lax.rem(core * 2 + 2, 4))
        have_tok(1 - g, 0, lax.rem(core * 2 + 3, 4))
        lift_most(1 - g)
        hand_on(1, x_peer)
        have_tok(1 - g, 1, core_peer)
        have_tok(1 - g, 1, cross_peer)
        lift_most(3 - g)
        for c in range(np_):
            arrived(0, outer2, c)
        for b in (g, 2 + g, 1 - g, 3 - g):
            lift_rest(b)
        scales()

        mine, theirs = at(core, 2 * rows), at(1 - core, 2 * rows)
        here, there = at(g, rows), at(1 - g, rows)

        def project(i):
            zz, k, w, _ = units[i]
            b = zz * np_ + k
            weights = down[b] if w == 1 else jnp.concatenate([down[b + j] for j in range(w)], axis=1)
            product = jnp.dot(hid[theirs, :], weights, preferred_element_type=f32).astype(bf)
            for j in range(w):
                core_out[b + j] = product[:, j * dc:(j + 1) * dc]
            go(remote(part(core_out, i), part(core_in, i), fresh(), core_recv.at[i], next_core))
            keep[i % 3, :, pl.ds(0, w * dc)] = jnp.dot(hid[mine, :], weights, preferred_element_type=f32)

        def fold(i):
            zz, k, w, _ = units[i]
            remote(part(core_out, i), part(core_in, i), 0, core_recv.at[i], next_core).wait_recv()
            for j in range(w):
                b, lanes = zz * np_ + k + j, pl.ds(j * dc, dc)
                y_out[b] = (keep[i % 3, there, lanes] + core_in[b, there, :].astype(f32)).astype(bf)
            go(remote(part(y_out, i), part(y_in, i), fresh(), y_recv.at[i], beside))
            for j in range(w):
                b, lanes = zz * np_ + k + j, pl.ds(j * dc, dc)
                keep[i % 3, here, lanes] = keep[i % 3, here, lanes] + core_in[b, here, :].astype(f32)

        away = {"fs": jnp.where(core == 0, z, outer), "tp": jnp.where(core == 0, x_peer, t)}

        def add(i):
            zz, k, w, _ = units[i]
            remote(part(y_out, i), part(y_in, i), 0, y_recv.at[i], beside).wait_recv()
            for j in range(w):
                b, lanes = zz * np_ + k + j, pl.ds(j * dc, dc)
                xz_out[b] = (keep[i % 3, here, lanes] + y_in[b].astype(f32)).astype(bf)
            go(remote(part(xz_out, i), part(x_in, i), fresh(), x_recv.at[i], away))

        def finish(i):
            @pl.when(core == 0)
            def _():
                remote(part(xz_out, i), part(x_in, i), 0, x_recv.at[i], away).wait_recv()
                value(i, xz_out, x_in)
                share(i).start()

        for i in range(n + 3):
            if 0 <= i - 1 < n:
                fold(i - 1)
            if i < n:
                zz, k, w, j = units[i]
                if j:
                    for c in range(k, k + w):
                        if j > 1:
                            arrived(1, zz, c)
                project(i)
            if i < 2:
                forward(1, 2 * i)
                forward(1, 2 * i + 1)
            if 0 <= i - 2 < n:
                add(i - 2)
            if 0 <= i - 3 < n:
                finish(i - 3)
        for copy in started[mark:]:
            copy.wait_send()
        del started[mark:]

        @pl.when(core == 0)
        def _():
            for i in range(n):
                share(i).wait_send()

        @pl.when(core == 1)
        def _():
            for i in range(n):
                share(i).wait_recv()

    for copy in started:
        copy.wait_send()

    step = 64

    def result(i):
        place = pl.ds(pl.multiple_of(i * step, step), step)
        return pltpu.make_async_copy(res.at[place, :], out.at[place, :], out_sem.at[i])

    def close(i, _):
        place = pl.ds(pl.multiple_of(i * step, step), step)
        row = jnp.concatenate([branch[b, place, :] for b in range(4 * np_)], axis=1).astype(f32)
        res[place, :] = (res[place, :].astype(f32) + rms_rows(row, post_gain[...])).astype(bf)
        result(i).start()
        return 0

    lax.fori_loop(0, rows // step, close, 0)
    for i in range(rows // step):
        result(i).wait()


def fused(tokens, pre_gain, up_weight, up_scale, down_weight, down_scale, post_gain):
    rows, width = tokens.shape
    depth, ff = up_weight.shape
    half, dc = ff // 2, depth // PIECES
    pieces = 4 * PIECES
    n = sum(len(w) for w in WIDTHS)
    bf, f32 = jnp.bfloat16, jnp.float32
    dma = pltpu.SemaphoreType.DMA
    anywhere, vmem = pl.BlockSpec(memory_space=pl.ANY), pl.BlockSpec(memory_space=pltpu.VMEM)
    return pl.pallas_call(
        kernel,
        out_shape=jax.ShapeDtypeStruct((rows, width), bf),
        in_specs=[anywhere, anywhere, anywhere, vmem, vmem, vmem, vmem],
        out_specs=anywhere,
        scratch_shapes=[
            pltpu.VMEM((rows, width), bf),
            pltpu.VMEM((depth, half), f32),
            pltpu.VMEM((half, depth), f32),
            pltpu.VMEM((width, half), bf),
            pltpu.VMEM((pieces, half, dc), bf),
            pltpu.VMEM((4 * rows, width), bf),
            pltpu.VMEM((4 * rows, half), f32),
            pltpu.VMEM((4 * rows, half), bf),
            pltpu.VMEM((4, 1, depth), f32),
            pltpu.VMEM((3, 2 * rows, 2 * dc), f32),
            pltpu.VMEM((pieces, 2 * rows, dc), bf),
            pltpu.VMEM((pieces, 2 * rows, dc), bf),
            pltpu.VMEM((pieces, rows, dc), bf),
            pltpu.VMEM((pieces, rows, dc), bf),
            pltpu.VMEM((pieces, rows, dc), bf),
            pltpu.VMEM((pieces, rows, dc), bf),
            pltpu.VMEM((pieces, rows, dc), bf),
            dma((144,)),
            dma((4, PIECES)),
            dma((4, PIECES)),
            dma((4, PIECES)),
            dma((4,)),
            dma((n,)),
            dma((n,)),
            dma((n,)),
            dma((n,)),
            dma((2, PIECES)),
            dma((2,)),
            dma((8,)),
        ],
        compiler_params=pltpu.CompilerParams(
            collective_id=0, has_side_effects=True, vmem_limit_bytes=60 << 20
        ),
    )(tokens, up_weight, down_weight, up_scale.reshape(1, ff), down_scale.reshape(1, depth),
      pre_gain.reshape(1, width), post_gain.reshape(1, width))


def solution(mesh):
    placed = (P(("grp", "fs"), None), P(), P("fs", "tp"), P("tp"), P("tp", "fs"), P("fs"), P())
    sizes = mesh.shape
    line = sizes["grp"] == 2 and sizes["fs"] == 4 and sizes["tp"] == 4
    return jax.shard_map(
        fused if line else plain, mesh=mesh, in_specs=placed, out_specs=P(("grp", "fs"), None), check_vma=False
    )
```

```python
import jax
import jax.numpy as jnp
from jax import lax
from jax.experimental import pallas as pl
from jax.experimental.pallas import tpu as pltpu
from jax.sharding import PartitionSpec as P

epsilon = 1e-06
MESH = pl.DeviceIdType.MESH
PIECES = 4
WIDTHS = ((2, 2), (2, 2), (2, 2), (2, 1, 1))
RAW = (0, 1, 0, 1, 0, 1, 2, 2, 2)
ARRIVAL = (1, 0, 3, 2, 5, 4, 6, 7, 8)


def rms_rows(values, scaling):
    return values * lax.rsqrt(jnp.mean(values * values, axis=-1, keepdims=True) + epsilon) * scaling


def activate(lifted, up_scale):
    return jnp.square(jax.nn.relu(lifted * up_scale)).astype(jnp.bfloat16)


def plain(tokens, pre_gain, up_weight, up_scale, down_weight, down_scale, post_gain):
    residual = tokens.astype(jnp.float32)
    normed = rms_rows(residual, pre_gain).astype(jnp.bfloat16)
    up_cast = up_weight.astype(jnp.bfloat16)
    down_cast = down_weight.astype(jnp.bfloat16)
    column_scales = lax.all_gather(down_scale, "fs", axis=0, tiled=True)
    up_full, down_full = (
        lax.all_gather(up_cast, "fs", axis=0, tiled=True),
        lax.all_gather(down_cast, "fs", axis=1, tiled=True),
    )
    lifted = jnp.dot(normed, up_full, preferred_element_type=jnp.float32)
    hidden = activate(lifted, up_scale)
    partials = jnp.dot(hidden, down_full, preferred_element_type=jnp.float32)
    partials = (partials * column_scales).astype(jnp.bfloat16)
    summed = lax.psum(partials, "tp").astype(jnp.float32)
    branch = lax.optimization_barrier(summed.astype(jnp.bfloat16)).astype(jnp.float32)
    return (residual + rms_rows(branch, post_gain)).astype(jnp.bfloat16)


def kernel(tokens, up_in, down_in, up_scale, down_scale, pre_gain, post_gain, out, res, up_f32, down_f32, up, down,
           tok, acc, hid, scl, keep, core_out, core_in, y_out, y_in, xz_out, x_in, branch, send, up_recv, down_recv,
           tok_recv, scl_recv, core_recv, y_recv, x_recv, raw_recv, br_recv,
           local, one_sem):
    g, z, t = lax.axis_index("grp"), lax.axis_index("fs"), lax.axis_index("tp")
    core, x = lax.rem(t, 2), t // 2
    pair = z // 2
    outer, inner, other = 3 * pair, 1 + pair, 2 - pair
    outer2 = 3 - outer
    is_outer = z == outer
    n_tp, np_ = 4, PIECES
    rows, width = tokens.shape
    depth, half = up_in.shape[0], up_in.shape[1] // 2
    du, dc, quarter = depth // np_, depth // np_, rows // np_
    core_peer, x_peer, cross_peer = x * 2 + 1 - core, (1 - x) * 2 + core, (1 - x) * 2 + 1 - core
    bf, f32 = jnp.bfloat16, jnp.float32

    def at(i, size):
        return pl.ds(pl.multiple_of(i * size, size), size)

    def load(kind, c):
        if kind == 0:
            copy = up_in.at[pl.ds(c * du, du), at(g, half)], up_f32.at[pl.ds(c * du, du), :]
        else:
            copy = down_in.at[at(g, half), :], down_f32
        return pltpu.make_async_copy(*copy, local.at[np_ if kind else c])

    load(0, 0).start()
    fetch = pltpu.make_async_copy(tokens, res, one_sem.at[0])
    fetch.start()
    for c in range(1, np_):
        load(0, c).start()
    load(1, 0).start()

    barrier = pltpu.get_barrier_semaphore()
    peers = [{"fs": lax.rem(z + o, 4)} for o in range(1, 4)] + [{"grp": 1 - g}]
    peers += [{"tp": lax.rem(t + o, n_tp)} for o in range(1, n_tp)]
    peers += [{"grp": 1 - g, "fs": z + 1 - 2 * lax.rem(z, 2)}]
    for peer in peers:
        pl.semaphore_signal(barrier, inc=1, device_id=peer, device_id_type=MESH)
    pl.semaphore_wait(barrier, len(peers))

    def remote(src, dst, s, r, peer):
        return pltpu.make_async_remote_copy(src_ref=src, dst_ref=dst, send_sem=send.at[s], recv_sem=r,
                                            device_id=peer, device_id_type=MESH)

    def same(ref, s, r, peer):
        return remote(ref, ref, s, r, peer)

    def slot(kind, zz, c, stage):
        if kind == 0:
            return up.at[at(zz * np_ + c, du), :], up_recv.at[c if stage == 0 else 3 + stage]
        mark = 2 * stage + c // 4 if stage < 2 or c < 4 else 5 + max(0, c - 5)
        return down.at[zz * np_ + c // 2, pl.ds(c % 2 * (half // 2), half // 2), :], down_recv.at[mark]

    def cast(kind, c):
        if kind == 0 or c == 0:
            load(kind, c).wait()
        if kind == 0:
            up[at(z * np_ + c, du), :] = up_f32[pl.ds(c * du, du), :].astype(bf)
        else:
            down[z * np_ + c] = down_f32[:, pl.ds(c * dc, dc)].astype(bf)

    def weight(kind, zz, c, stage, s, peer):
        ref, r = slot(kind, zz, c, stage)
        same(ref, s, r, peer).start()

    def took(ref, r):
        same(ref, 0, r, {"fs": other}).wait_recv()

    def gave(ref, s):
        same(ref, s, scl_recv.at[0], {"fs": other}).wait_send()

    def piece(gg, kind, k):
        b = kind * 2 + gg
        return tok.at[at(b * np_ + k, quarter), :], tok_recv.at[b, k]

    def pass_tok(gg, kind, k, peer):
        ref, r = piece(gg, kind, k)
        same(ref, 1, r, peer).start()

    def have_tok(gg, kind, k):
        took(*piece(gg, kind, k))

    def norm(b, k):
        def one(i, _):
            source = pl.ds(pl.multiple_of(k * quarter + i * 64, 64), 64)
            target = pl.ds(pl.multiple_of((b * np_ + k) * quarter + i * 64, 64), 64)
            tok[target, :] = rms_rows(res[source, :].astype(f32), pre_gain[...]).astype(bf)
            return 0
        lax.fori_loop(0, quarter // 64, one, 0)

    blocks = (inner, outer, other, outer2)
    units = []
    for j, widths in enumerate(WIDTHS):
        k = 0
        for w in widths:
            units.append((blocks[j], k, w, j))
            k += w
    n = len(units)

    def total(*modes):
        return sum(u[2] for u, raw in zip(units, RAW) if raw in modes)

    def part(ref, i):
        zz, k, w, _ = units[i]
        return ref.at[pl.ds(zz * np_ + k, w)]

    mine_rows, their_rows = at(g, rows), at(1 - g, rows)

    def half_of(ref, i, lines):
        zz, k, w, _ = units[i]
        return ref.at[pl.ds(zz * np_ + k, w), lines, :]

    def raw_half(i, own, s):
        lines = mine_rows if own else their_rows
        ref = half_of(core_in, i, lines)
        return same(ref, s, (raw_recv if own else core_recv).at[i], {"fs": outer})

    def value(i, first, second):
        zz, k, w, _ = units[i]
        for j in range(w):
            b = zz * np_ + k + j
            total = first[b].astype(f32) + second[b].astype(f32)
            branch[b] = (total * scl[zz, :, pl.ds((k + j) * dc, dc)]).astype(bf)

    def share(i):
        return same(part(branch, i), 2, br_recv.at[0], {"tp": core_peer})

    for o in range(1, 4):
        remote(down_scale, scl.at[z], 0, scl_recv.at[0], {"fs": lax.rem(z + o, 4)}).start()
    own_scale = pltpu.make_async_copy(down_scale, scl.at[z], one_sem.at[1])
    own_scale.start()

    def scales():
        own_scale.wait()
        took(scl.at[pl.ds(0, 3)], scl_recv.at[0])

    @pl.when(is_outer)
    def _():
        to = {"fs": inner}
        fetch.wait()
        norm(2 + g, t)
        pass_tok(g, 1, t, to)
        for c in range(np_):
            cast(0, c)
            weight(0, z, c, 0, 3, to)
        for c in range(np_):
            cast(1, c)
            for k in range(2):
                weight(1, z, 2 * c + k, 0, 4, to)
        scales()

        @pl.when(core == 1)
        def _():
            def relay(i):
                return remote(part(x_in, i), part(y_in, i), 5, y_recv.at[i], {"tp": x_peer})

            def side(i):
                return remote(half_of(core_in, i, their_rows), part(y_in, i), 6, y_recv.at[i], {"grp": 1 - g})

            def swap(i):
                return remote(part(xz_out, i), part(x_in, i), 7, x_recv.at[i], {"tp": x_peer})

            def first(i):
                if RAW[i] == 2:
                    raw_half(i, True, 0).wait_recv()
                elif RAW[i]:
                    raw_half(i, False, 0).wait_recv()
                    side(i).start()
                else:
                    remote(part(x_in, i), part(x_in, i), 0, x_recv.at[i], {"fs": inner}).wait_recv()
                    relay(i).start()

            def second(i):
                zz, k, w, _ = units[i]
                if RAW[i] == 1:
                    raw_half(i, True, 0).wait_recv()
                side(i).wait_recv()
                for j in range(w):
                    b = zz * np_ + k + j
                    xz_out[b] = (core_in[b, mine_rows, :].astype(f32) + y_in[b].astype(f32)).astype(bf)
                swap(i).start()

            def third(i):
                if RAW[i]:
                    swap(i).wait_recv()
                    value(i, xz_out, x_in)
                else:
                    relay(i).wait_recv()
                    value(i, x_in, y_in)
                share(i).start()

            for s in range(n + 2):
                if s < n:
                    first(ARRIVAL[s])
                if 0 <= s - 1 < n:
                    i = ARRIVAL[s - 1]
                    if RAW[i]:
                        second(i)
                    else:
                        third(i)
                if 0 <= s - 2 < n and RAW[ARRIVAL[s - 2]]:
                    third(ARRIVAL[s - 2])
            gave(x_in.at[pl.ds(0, total(0))], 5)
            gave(x_in.at[pl.ds(0, total(1))], 6)
            gave(x_in.at[pl.ds(0, total(1, 2))], 7)
            gave(branch, 2)

        @pl.when(core == 0)
        def _():
            took(branch, br_recv.at[0])

        gave(tok.at[pl.ds(0, quarter), :], 1)
        gave(up.at[pl.ds(0, depth), :], 3)
        gave(down.at[pl.ds(0, np_)], 4)

    @pl.when(jnp.logical_not(is_outer))
    def _():
        across, beside, next_core = {"fs": other}, {"grp": 1 - g}, {"tp": core_peer}
        for c in range(np_):
            cast(0, c)
            weight(0, z, c, 1, 3, across)
        fetch.wait()
        for j in range(np_):
            k = lax.rem(core * 2 + j, 4)
            norm(g, k)
            if j < 2:
                pass_tok(g, 0, k, beside)
        for c in range(np_):
            cast(1, c)

        have_tok(g, 1, t)
        for peer in ({"tp": x_peer}, beside, next_core, {"tp": cross_peer}):
            pass_tok(g, 1, t, peer)

        def forward(c):
            took(*slot(0, outer, c, 0))
            weight(0, outer, c, 2, 4, across)

        def forward_down(c):
            took(down.at[pl.ds(outer * np_ + 2 * c, 2)], down_recv.at[c])
            for k in range(4):
                weight(1, outer, 4 * c + k, 2, 6, across)

        def hand_on(kind, k):
            have_tok(1 - g, kind, k)
            pass_tok(1 - g, kind, k, next_core)

        forward(0)
        hand_on(0, core * 2)
        forward(1)
        hand_on(0, core * 2 + 1)
        have_tok(g, 1, x_peer)
        pass_tok(g, 1, x_peer, beside)
        forward(2)
        forward(3)
        for c in range(2 * np_):
            weight(1, z, c, 1, 5, across)

        tile = 512
        most = 3 * depth
        low, rest = pair * depth, outer2 * depth
        most_at = pl.ds(pl.multiple_of(low, depth), most)
        rest_at = pl.ds(pl.multiple_of(rest, depth), depth)

        def lift_most(b):
            lines = at(b, rows)

            def one(i, _):
                columns = at(i, tile)
                acc[lines, columns] = jnp.dot(tok[lines, most_at], up[most_at, columns], preferred_element_type=f32)
                return 0
            lax.fori_loop(0, half // tile, one, 0)

        def lift_all(b):
            lines = at(b, rows)

            def one(i, _):
                columns = at(i, tile)
                lifted = jnp.dot(tok[lines, :], up[:, columns], preferred_element_type=f32)
                whole = pl.ds(pl.multiple_of(g * half + i * tile, tile), tile)
                hid[lines, columns] = activate(lifted, up_scale[:, whole])
                return 0
            lax.fori_loop(0, half // tile, one, 0)

        def lift_rest(b):
            lines = at(b, rows)

            def one(i, _):
                columns = at(i, tile)
                lifted = acc[lines, columns] + jnp.dot(tok[lines, rest_at], up[rest_at, columns],
                                                       preferred_element_type=f32)
                whole = pl.ds(pl.multiple_of(g * half + i * tile, tile), tile)
                hid[lines, columns] = activate(lifted, up_scale[:, whole])
                return 0
            lax.fori_loop(0, half // tile, one, 0)

        took(up.at[at(other, depth), :], up_recv.at[4])
        lift_most(g)
        have_tok(g, 1, core_peer)
        have_tok(g, 1, cross_peer)
        lift_most(2 + g)
        hand_on(1, t)
        have_tok(1 - g, 0, lax.rem(core * 2 + 2, 4))
        have_tok(1 - g, 0, lax.rem(core * 2 + 3, 4))
        lift_most(1 - g)
        hand_on(1, x_peer)
        took(up.at[at(outer2, depth), :], up_recv.at[5])
        for b in (g, 2 + g, 1 - g):
            lift_rest(b)
        have_tok(1 - g, 1, core_peer)
        have_tok(1 - g, 1, cross_peer)
        lift_all(3 - g)
        scales()

        mine, theirs = at(core, 2 * rows), at(1 - core, 2 * rows)
        def project(i):
            zz, k, w, _ = units[i]
            b = zz * np_ + k
            weights = down[b] if w == 1 else jnp.concatenate([down[b + j] for j in range(w)], axis=1)
            product = jnp.dot(hid[theirs, :], weights, preferred_element_type=f32).astype(bf)
            for j in range(w):
                core_out[b + j] = product[:, j * dc:(j + 1) * dc]
            remote(part(core_out, i), part(core_in, i), 7, core_recv.at[i], next_core).start()
            keep[i % 3, :, pl.ds(0, w * dc)] = jnp.dot(hid[mine, :], weights, preferred_element_type=f32)

        def project_last(i):
            zz, k, _, _ = units[i]
            b = zz * np_ + k
            early, late = pl.ds(0, half // 2), pl.ds(half // 2, half // 2)
            lanes = pl.ds(0, dc)
            took(*slot(1, zz, 2 * k, 2))
            acc[pl.ds(0, 2 * rows), lanes] = jnp.dot(hid[theirs, early], down[b, early, :], preferred_element_type=f32)
            keep[i % 3, :, lanes] = jnp.dot(hid[mine, early], down[b, early, :], preferred_element_type=f32)
            took(*slot(1, zz, 2 * k + 1, 2))
            core_out[b] = (acc[pl.ds(0, 2 * rows), lanes] + jnp.dot(
                hid[theirs, late], down[b, late, :], preferred_element_type=f32)).astype(bf)
            remote(part(core_out, i), part(core_in, i), 7, core_recv.at[i], next_core).start()
            keep[i % 3, :, lanes] = keep[i % 3, :, lanes] + jnp.dot(
                hid[mine, late], down[b, late, :], preferred_element_type=f32)

        away = {"fs": jnp.where(core == 0, z, outer), "tp": jnp.where(core == 0, x_peer, t)}

        def by_y(i):
            return remote(part(y_out, i), part(y_in, i), 8, y_recv.at[i], beside)

        def direct(i):
            return remote(half_of(core_in, i, their_rows), part(y_in, i), 10, y_recv.at[i],
                          {"grp": 1 - g, "fs": outer})

        def sent_away(i):
            return remote(part(xz_out, i), part(x_in, i), 9, x_recv.at[i], away)

        def fold(i):
            zz, k, w, _ = units[i]
            remote(part(core_out, i), part(core_in, i), 0, core_recv.at[i], next_core).wait_recv()

            def pieces(lines):
                for j in range(w):
                    b = zz * np_ + k + j
                    yield b, keep[i % 3, lines, pl.ds(j * dc, dc)] + core_in[b, lines, :].astype(f32)

            def through_y():
                for b, total in pieces(their_rows):
                    y_out[b] = total.astype(bf)
                by_y(i).start()
                for j in range(w):
                    b, lanes = zz * np_ + k + j, pl.ds(j * dc, dc)
                    keep[i % 3, mine_rows, lanes] = (keep[i % 3, mine_rows, lanes]
                                                     + core_in[b, mine_rows, :].astype(f32))

            if not RAW[i]:
                through_y()
                return

            @pl.when(core == 0)
            def _():
                through_y()

            @pl.when(core == 1)
            def _():
                for own in range(2):
                    lines = mine_rows if own else their_rows
                    for b, total in pieces(lines):
                        core_in[b, lines, :] = total.astype(bf)
                    if RAW[i] == 2 and not own:
                        direct(i).start()
                    else:
                        raw_half(i, own, 10).start()

        def add(i):
            zz, k, w, _ = units[i]

            def through_x():
                by_y(i).wait_recv()
                for j in range(w):
                    b, lanes = zz * np_ + k + j, pl.ds(j * dc, dc)
                    xz_out[b] = (keep[i % 3, mine_rows, lanes] + y_in[b].astype(f32)).astype(bf)
                sent_away(i).start()

            if not RAW[i]:
                through_x()
                return

            @pl.when(core == 0)
            def _():
                through_x()

        def finish(i):
            @pl.when(core == 0)
            def _():
                sent_away(i).wait_recv()
                value(i, xz_out, x_in)
                share(i).start()

        def ready(i):
            zz, k, w, j = units[i]
            if j > 1:
                took(down.at[pl.ds(zz * np_ + k, w)], slot(1, zz, 2 * k, j - 1)[1])

        for i in range(n):
            eager = units[i][3] == 3
            if i and not eager:
                fold(i - 1)
            if eager and units[i - 1][3] < 3:
                fold(i - 1)
                add(i - 2)
                finish(i - 3)
            if i == n - 1:
                project_last(i)
            else:
                ready(i)
                project(i)
            if i < 2:
                forward_down(i)
            if eager:
                fold(i)
                add(i - 1)
                finish(i - 2)
            else:
                if i >= 2:
                    add(i - 2)
                if i >= 3:
                    finish(i - 3)
        add(n - 1)
        finish(n - 2)
        finish(n - 1)
        gave(tok.at[pl.ds(0, 11 * quarter), :], 1)
        for s in (3, 4):
            gave(up.at[pl.ds(0, depth), :], s)
        for s in (5, 6):
            gave(down.at[pl.ds(0, np_)], s)
        gave(core_out, 7)

        @pl.when(core == 0)
        def _():
            gave(y_out, 8)
            gave(xz_out, 9)
            gave(branch, 2)

        @pl.when(core == 1)
        def _():
            gave(y_out.at[pl.ds(0, total(0))], 8)
            gave(xz_out.at[pl.ds(0, total(0))], 9)
            gave(core_in.at[pl.ds(0, total(1, 2))], 10)
            took(branch, br_recv.at[0])

    gave(scl.at[pl.ds(0, 3)], 0)

    step = 64

    def result(i):
        place = pl.ds(pl.multiple_of(i * step, step), step)
        return pltpu.make_async_copy(res.at[place, :], out.at[place, :], one_sem.at[2])

    def close(i, _):
        place = pl.ds(pl.multiple_of(i * step, step), step)
        row = jnp.concatenate([branch[b, place, :] for b in range(4 * np_)], axis=1).astype(f32)
        res[place, :] = (res[place, :].astype(f32) + rms_rows(row, post_gain[...])).astype(bf)
        result(i).start()
        return 0

    lax.fori_loop(0, rows // step, close, 0)
    pltpu.make_async_copy(res, out, one_sem.at[2]).wait()


def fused(tokens, pre_gain, up_weight, up_scale, down_weight, down_scale, post_gain):
    rows, width = tokens.shape
    depth, ff = up_weight.shape
    half, dc = ff // 2, depth // PIECES
    pieces = 4 * PIECES
    n = sum(len(w) for w in WIDTHS)
    bf, f32 = jnp.bfloat16, jnp.float32
    dma = pltpu.SemaphoreType.DMA
    anywhere, vmem = pl.BlockSpec(memory_space=pl.ANY), pl.BlockSpec(memory_space=pltpu.VMEM)
    return pl.pallas_call(
        kernel,
        out_shape=jax.ShapeDtypeStruct((rows, width), bf),
        in_specs=[anywhere, anywhere, anywhere, vmem, vmem, vmem, vmem],
        out_specs=anywhere,
        scratch_shapes=[
            pltpu.VMEM((rows, width), bf),
            pltpu.VMEM((depth, half), f32),
            pltpu.VMEM((half, depth), f32),
            pltpu.VMEM((width, half), bf),
            pltpu.VMEM((pieces, half, dc), bf),
            pltpu.VMEM((4 * rows, width), bf),
            pltpu.VMEM((4 * rows, half), f32),
            pltpu.VMEM((4 * rows, half), bf),
            pltpu.VMEM((4, 1, depth), f32),
            pltpu.VMEM((3, 2 * rows, 2 * dc), f32),
            pltpu.VMEM((pieces, 2 * rows, dc), bf),
            pltpu.VMEM((pieces, 2 * rows, dc), bf),
            pltpu.VMEM((pieces, rows, dc), bf),
            pltpu.VMEM((pieces, rows, dc), bf),
            pltpu.VMEM((pieces, rows, dc), bf),
            pltpu.VMEM((pieces, rows, dc), bf),
            pltpu.VMEM((pieces, rows, dc), bf),
            dma((11,)),
            dma((6,)),
            dma((8,)),
            dma((4, PIECES)),
            dma((1,)),
            dma((n,)),
            dma((n,)),
            dma((n,)),
            dma((n,)),
            dma((1,)),
            dma((PIECES + 1,)),
            dma((3,)),
        ],
        compiler_params=pltpu.CompilerParams(
            collective_id=0, has_side_effects=True, vmem_limit_bytes=60 << 20
        ),
    )(tokens, up_weight, down_weight, up_scale.reshape(1, ff), down_scale.reshape(1, depth),
      pre_gain.reshape(1, width), post_gain.reshape(1, width))


def solution(mesh):
    placed = (P(("grp", "fs"), None), P(), P("fs", "tp"), P("tp"), P("tp", "fs"), P("fs"), P())
    sizes = mesh.shape
    line = sizes["grp"] == 2 and sizes["fs"] == 4 and sizes["tp"] == 4
    return jax.shard_map(
        fused if line else plain, mesh=mesh, in_specs=placed, out_specs=P(("grp", "fs"), None), check_vma=False
    )
```

```python
import jax
import jax.numpy as jnp
from jax import lax
from jax.experimental import pallas as pl
from jax.experimental.pallas import tpu as pltpu
from jax.sharding import PartitionSpec as P

epsilon = 1e-06
MESH = pl.DeviceIdType.MESH
PIECES = 4
WIDTHS = ((2, 2), (2, 2), (2, 2), (2, 1, 1))
RAW = (0, 1, 0, 1, 0, 1, 2, 2, 2)
ORDER = ("P0F0P1F1P2F2A0P3F3A1N0P4F4A2P5F5A3N1", "A4N2P6F6A5N3P7F7A6N4P8F8A7N5A8N6N7N8")
STEPS = tuple(part[i:i + 2] for part in ORDER for i in range(0, len(part), 2))
ARRIVAL = tuple(int(s[1:]) for s in STEPS if s[0] == "AFFA"[RAW[int(s[1:])]])


def rms_rows(values, scaling):
    return values * lax.rsqrt(jnp.mean(values * values, axis=-1, keepdims=True) + epsilon) * scaling


def activate(lifted, up_scale):
    return jnp.square(jax.nn.relu(lifted * up_scale)).astype(jnp.bfloat16)


def plain(tokens, pre_gain, up_weight, up_scale, down_weight, down_scale, post_gain):
    residual = tokens.astype(jnp.float32)
    normed = rms_rows(residual, pre_gain).astype(jnp.bfloat16)
    up_cast = up_weight.astype(jnp.bfloat16)
    down_cast = down_weight.astype(jnp.bfloat16)
    column_scales = lax.all_gather(down_scale, "fs", axis=0, tiled=True)
    up_full, down_full = (
        lax.all_gather(up_cast, "fs", axis=0, tiled=True),
        lax.all_gather(down_cast, "fs", axis=1, tiled=True),
    )
    lifted = jnp.dot(normed, up_full, preferred_element_type=jnp.float32)
    hidden = activate(lifted, up_scale)
    partials = jnp.dot(hidden, down_full, preferred_element_type=jnp.float32)
    partials = (partials * column_scales).astype(jnp.bfloat16)
    summed = lax.psum(partials, "tp").astype(jnp.float32)
    branch = lax.optimization_barrier(summed.astype(jnp.bfloat16)).astype(jnp.float32)
    return (residual + rms_rows(branch, post_gain)).astype(jnp.bfloat16)


def kernel(tokens, up_in, down_in, up_scale, down_scale, pre_gain, out, res, up_f32, down_f32, up, down,
           tok, acc, hid, scl, keep, core_out, core_in, y_out, y_in, xz_out, x_in, branch, send, up_recv, down_recv,
           tok_recv, scl_recv, core_recv, y_recv, x_recv, raw_recv, br_recv,
           local, one_sem):
    g, z, t = lax.axis_index("grp"), lax.axis_index("fs"), lax.axis_index("tp")
    core, x = lax.rem(t, 2), t // 2
    pair = z // 2
    outer, inner, other = 3 * pair, 1 + pair, 2 - pair
    outer2 = 3 - outer
    is_outer = z == outer
    n_tp, np_ = 4, PIECES
    rows, width = tokens.shape
    depth, half = up_in.shape[0], up_in.shape[1] // 2
    du, dc, quarter = depth // np_, depth // np_, rows // np_
    core_peer, x_peer, cross_peer = x * 2 + 1 - core, (1 - x) * 2 + core, (1 - x) * 2 + 1 - core
    bf, f32 = jnp.bfloat16, jnp.float32

    def at(i, size):
        return pl.ds(pl.multiple_of(i * size, size), size)

    def load(kind, c):
        if kind == 0:
            copy = up_in.at[pl.ds(c * du, du), at(g, half)], up_f32.at[pl.ds(c * du, du), :]
        else:
            copy = down_in.at[at(g, half), :], down_f32
        return pltpu.make_async_copy(*copy, local.at[np_ if kind else c])

    load(0, 0).start()
    fetch = pltpu.make_async_copy(tokens, res, one_sem.at[0])
    fetch.start()
    for c in range(1, np_):
        load(0, c).start()
    load(1, 0).start()

    barrier = pltpu.get_barrier_semaphore()
    peers = [{"fs": lax.rem(z + o, 4)} for o in range(1, 4)] + [{"grp": 1 - g}]
    peers += [{"tp": lax.rem(t + o, n_tp)} for o in range(1, n_tp)]
    peers += [{"grp": 1 - g, "fs": z + 1 - 2 * lax.rem(z, 2)}]
    for peer in peers:
        pl.semaphore_signal(barrier, inc=1, device_id=peer, device_id_type=MESH)
    pl.semaphore_wait(barrier, len(peers))

    def remote(src, dst, s, r, peer):
        return pltpu.make_async_remote_copy(src_ref=src, dst_ref=dst, send_sem=send.at[s], recv_sem=r,
                                            device_id=peer, device_id_type=MESH)

    def same(ref, s, r, peer):
        return remote(ref, ref, s, r, peer)

    def slot(kind, zz, c, stage):
        if kind == 0:
            return up.at[at(zz * np_ + c, du), :], up_recv.at[c if stage == 0 else 3 + stage]
        mark = 2 * stage + c // 4 if stage < 2 or c < 4 else 5 + max(0, c - 5)
        return down.at[zz * np_ + c // 2, pl.ds(c % 2 * (half // 2), half // 2), :], down_recv.at[mark]

    def cast(kind, c):
        if kind == 0 or c == 0:
            load(kind, c).wait()
        if kind == 0:
            up[at(z * np_ + c, du), :] = up_f32[pl.ds(c * du, du), :].astype(bf)
        else:
            down[z * np_ + c] = down_f32[:, pl.ds(c * dc, dc)].astype(bf)

    def weight(kind, zz, c, stage, s, peer):
        ref, r = slot(kind, zz, c, stage)
        same(ref, s, r, peer).start()

    def took(ref, r):
        same(ref, 0, r, {"fs": other}).wait_recv()

    def gave(ref, s):
        same(ref, s, scl_recv.at[0], {"fs": other}).wait_send()

    def piece(gg, kind, k):
        b = kind * 2 + gg
        return tok.at[at(b * np_ + k, quarter), :], tok_recv.at[b, k]

    def pass_tok(gg, kind, k, peer):
        ref, r = piece(gg, kind, k)
        same(ref, 1, r, peer).start()

    def have_tok(gg, kind, k):
        took(*piece(gg, kind, k))

    def norm(b, k):
        def one(i, _):
            source = pl.ds(pl.multiple_of(k * quarter + i * 64, 64), 64)
            target = pl.ds(pl.multiple_of((b * np_ + k) * quarter + i * 64, 64), 64)
            tok[target, :] = rms_rows(res[source, :].astype(f32), pre_gain[...]).astype(bf)
            return 0
        lax.fori_loop(0, quarter // 64, one, 0)

    blocks = (inner, outer, other, outer2)
    units = []
    for j, widths in enumerate(WIDTHS):
        k = 0
        for w in widths:
            units.append((blocks[j], k, w, j))
            k += w
    n = len(units)

    def total(*modes):
        return sum(u[2] for u, raw in zip(units, RAW) if raw in modes)

    def part(ref, i):
        zz, k, w, _ = units[i]
        return ref.at[pl.ds(zz * np_ + k, w)]

    mine_rows, their_rows = at(g, rows), at(1 - g, rows)

    def half_of(ref, i, lines):
        zz, k, w, _ = units[i]
        return ref.at[pl.ds(zz * np_ + k, w), lines, :]

    fold_rows = rows // 2

    def strip(ref, i, gg):
        return half_of(ref, i, at(gg, fold_rows))

    def raw_half(i, own, s):
        lines = mine_rows if own else their_rows
        ref = half_of(core_in, i, lines)
        return same(ref, s, (raw_recv if own else core_recv).at[i], {"fs": outer})

    def value(i, first, second):
        zz, k, w, _ = units[i]
        for j in range(w):
            b = zz * np_ + k + j
            total = first[b].astype(f32) + second[b].astype(f32)
            branch[b] = (total * scl[zz, :, pl.ds((k + j) * dc, dc)]).astype(bf)

    def write(i):
        pltpu.make_async_copy(part(branch, i), part(out, i), one_sem.at[2]).start()

    def receive(order):
        for i in order:
            took(part(branch, i), br_recv.at[i])
            write(i)

    def share(i):
        return same(part(branch, i), 2, br_recv.at[i], {"tp": core_peer})

    for o in range(1, 4):
        remote(down_scale, scl.at[z], 0, scl_recv.at[0], {"fs": lax.rem(z + o, 4)}).start()
    own_scale = pltpu.make_async_copy(down_scale, scl.at[z], one_sem.at[1])
    own_scale.start()

    def scales():
        own_scale.wait()
        took(scl.at[pl.ds(0, 3)], scl_recv.at[0])

    @pl.when(is_outer)
    def _():
        to = {"fs": inner}
        fetch.wait()
        norm(2 + g, t)
        pass_tok(g, 1, t, to)
        for c in range(np_):
            cast(0, c)
            weight(0, z, c, 0, 3, to)
        for c in range(np_):
            cast(1, c)
            for k in range(2):
                weight(1, z, 2 * c + k, 0, 4, to)
        scales()

        @pl.when(core == 1)
        def _():
            def relay(i):
                return remote(part(x_in, i), part(y_in, i), 5, y_recv.at[i], {"tp": x_peer})

            def side(i):
                return remote(half_of(core_in, i, their_rows), part(y_in, i), 6, y_recv.at[i], {"grp": 1 - g})

            def swap(i):
                return remote(part(xz_out, i), part(x_in, i), 7, x_recv.at[i], {"tp": x_peer})

            def side_strip(i):
                return remote(strip(x_in, i, 1 - g), strip(y_in, i, 0), 9, y_recv.at[i], {"grp": 1 - g})

            def swap_strip(i, xx):
                return same(strip(branch, i, xx), 8, x_recv.at[i], {"tp": x_peer})

            def first(i):
                if RAW[i] == 3:
                    took(strip(x_in, i, 1 - g), core_recv.at[i])
                    side_strip(i).start()
                elif RAW[i] == 2:
                    raw_half(i, True, 0).wait_recv()
                elif RAW[i]:
                    raw_half(i, False, 0).wait_recv()
                    side(i).start()
                else:
                    remote(part(x_in, i), part(x_in, i), 0, x_recv.at[i], {"fs": inner}).wait_recv()
                    relay(i).start()

            def second(i):
                zz, k, w, _ = units[i]
                if RAW[i] == 3:
                    took(strip(x_in, i, g), raw_recv.at[i])
                    side_strip(i).wait_recv()
                    for j in range(w):
                        b = zz * np_ + k + j
                        both = x_in[b, at(g, fold_rows), :].astype(f32) + y_in[b, pl.ds(0, fold_rows), :].astype(f32)
                        branch[b, at(x, fold_rows), :] = (both * scl[zz, :, pl.ds((k + j) * dc, dc)]).astype(bf)
                    swap_strip(i, x).start()
                    return
                if RAW[i] == 1:
                    raw_half(i, True, 0).wait_recv()
                side(i).wait_recv()
                for j in range(w):
                    b = zz * np_ + k + j
                    xz_out[b] = (core_in[b, mine_rows, :].astype(f32) + y_in[b].astype(f32)).astype(bf)
                swap(i).start()

            def third(i):
                if RAW[i] == 3:
                    swap_strip(i, 1 - x).wait_recv()
                elif RAW[i]:
                    swap(i).wait_recv()
                    value(i, xz_out, x_in)
                else:
                    relay(i).wait_recv()
                    value(i, x_in, y_in)
                share(i).start()
                write(i)

            for s in range(n + 2):
                if s < n:
                    first(ARRIVAL[s])
                if 0 <= s - 1 < n:
                    i = ARRIVAL[s - 1]
                    if RAW[i]:
                        second(i)
                    else:
                        third(i)
                if 0 <= s - 2 < n and RAW[ARRIVAL[s - 2]]:
                    third(ARRIVAL[s - 2])
            gave(x_in.at[pl.ds(0, total(0))], 5)
            if total(1):
                gave(x_in.at[pl.ds(0, total(1))], 6)
            if total(3):
                for s in (8, 9):
                    gave(x_in.at[pl.ds(0, total(3)), pl.ds(0, fold_rows), :], s)
            gave(x_in.at[pl.ds(0, total(1, 2))], 7)
            gave(branch, 2)

        @pl.when(core == 0)
        def _():
            receive(ARRIVAL)

        gave(tok.at[pl.ds(0, quarter), :], 1)
        gave(up.at[pl.ds(0, depth), :], 3)
        gave(down.at[pl.ds(0, np_)], 4)

    @pl.when(jnp.logical_not(is_outer))
    def _():
        across, beside, next_core = {"fs": other}, {"grp": 1 - g}, {"tp": core_peer}
        for c in range(np_):
            cast(0, c)
            weight(0, z, c, 1, 3, across)
        fetch.wait()
        for j in range(np_):
            k = lax.rem(core * 2 + j, 4)
            norm(g, k)
            if j < 2:
                pass_tok(g, 0, k, beside)
        for c in range(np_):
            cast(1, c)

        have_tok(g, 1, t)
        for peer in ({"tp": x_peer}, beside, next_core, {"tp": cross_peer}):
            pass_tok(g, 1, t, peer)

        def forward(c):
            took(*slot(0, outer, c, 0))
            weight(0, outer, c, 2, 4, across)

        def forward_down(c):
            took(down.at[pl.ds(outer * np_ + 2 * c, 2)], down_recv.at[c])
            for k in range(4):
                weight(1, outer, 4 * c + k, 2, 6, across)

        def hand_on(kind, k):
            have_tok(1 - g, kind, k)
            pass_tok(1 - g, kind, k, next_core)

        forward(0)
        hand_on(0, core * 2)
        forward(1)
        hand_on(0, core * 2 + 1)
        have_tok(g, 1, x_peer)
        pass_tok(g, 1, x_peer, beside)
        forward(2)
        forward(3)
        for c in range(2 * np_):
            weight(1, z, c, 1, 5, across)

        tile = 512
        most = 3 * depth
        low, rest = pair * depth, outer2 * depth
        most_at = pl.ds(pl.multiple_of(low, depth), most)
        rest_at = pl.ds(pl.multiple_of(rest, depth), depth)

        def lift_most(b):
            lines = at(b, rows)

            def one(i, _):
                columns = at(i, tile)
                acc[lines, columns] = jnp.dot(tok[lines, most_at], up[most_at, columns], preferred_element_type=f32)
                return 0
            lax.fori_loop(0, half // tile, one, 0)

        def lift_all(b):
            lines = at(b, rows)

            def one(i, _):
                columns = at(i, tile)
                lifted = jnp.dot(tok[lines, :], up[:, columns], preferred_element_type=f32)
                whole = pl.ds(pl.multiple_of(g * half + i * tile, tile), tile)
                hid[lines, columns] = activate(lifted, up_scale[:, whole])
                return 0
            lax.fori_loop(0, half // tile, one, 0)

        def lift_rest(b):
            lines = at(b, rows)

            def one(i, _):
                columns = at(i, tile)
                lifted = acc[lines, columns] + jnp.dot(tok[lines, rest_at], up[rest_at, columns],
                                                       preferred_element_type=f32)
                whole = pl.ds(pl.multiple_of(g * half + i * tile, tile), tile)
                hid[lines, columns] = activate(lifted, up_scale[:, whole])
                return 0
            lax.fori_loop(0, half // tile, one, 0)

        took(up.at[at(other, depth), :], up_recv.at[4])
        lift_most(g)
        have_tok(g, 1, core_peer)
        have_tok(g, 1, cross_peer)
        lift_most(2 + g)
        hand_on(1, t)
        have_tok(1 - g, 0, lax.rem(core * 2 + 2, 4))
        have_tok(1 - g, 0, lax.rem(core * 2 + 3, 4))
        lift_most(1 - g)
        hand_on(1, x_peer)
        took(up.at[at(outer2, depth), :], up_recv.at[5])
        for b in (g, 2 + g, 1 - g):
            lift_rest(b)
        have_tok(1 - g, 1, core_peer)
        have_tok(1 - g, 1, cross_peer)
        lift_all(3 - g)
        scales()

        mine, theirs = at(core, 2 * rows), at(1 - core, 2 * rows)
        def project(i):
            zz, k, w, _ = units[i]
            b = zz * np_ + k
            weights = down[b] if w == 1 else jnp.concatenate([down[b + j] for j in range(w)], axis=1)
            product = jnp.dot(hid[theirs, :], weights, preferred_element_type=f32).astype(bf)
            for j in range(w):
                core_out[b + j] = product[:, j * dc:(j + 1) * dc]
            keep[i % 3, :, pl.ds(0, w * dc)] = jnp.dot(hid[mine, :], weights, preferred_element_type=f32)
            remote(part(core_out, i), part(core_in, i), 7, core_recv.at[i], next_core).start()

        def project_last(i):
            zz, k, _, _ = units[i]
            b = zz * np_ + k
            early, late = pl.ds(0, half // 2), pl.ds(half // 2, half // 2)
            lanes = pl.ds(0, dc)
            took(*slot(1, zz, 2 * k, 2))
            acc[pl.ds(0, 2 * rows), lanes] = jnp.dot(hid[theirs, early], down[b, early, :], preferred_element_type=f32)
            keep[i % 3, :, lanes] = jnp.dot(hid[mine, early], down[b, early, :], preferred_element_type=f32)
            took(*slot(1, zz, 2 * k + 1, 2))
            core_out[b] = (acc[pl.ds(0, 2 * rows), lanes] + jnp.dot(
                hid[theirs, late], down[b, late, :], preferred_element_type=f32)).astype(bf)
            remote(part(core_out, i), part(core_in, i), 7, core_recv.at[i], next_core).start()
            keep[i % 3, :, lanes] = keep[i % 3, :, lanes] + jnp.dot(
                hid[mine, late], down[b, late, :], preferred_element_type=f32)

        away = {"fs": jnp.where(core == 0, z, outer), "tp": jnp.where(core == 0, x_peer, t)}

        def by_y(i):
            return remote(part(y_out, i), part(y_in, i), 8, y_recv.at[i], beside)

        def turn(i, gg):
            lines = pl.ds(pl.multiple_of(gg * rows + (1 - x) * fold_rows, fold_rows), fold_rows)
            return remote(half_of(core_in, i, lines), strip(y_in, i, gg), 11, y_recv.at[i], {"tp": x_peer})

        def direct(i):
            return remote(half_of(core_in, i, their_rows), part(y_in, i), 10, y_recv.at[i],
                          {"grp": 1 - g, "fs": outer})

        def sent_away(i):
            return remote(part(xz_out, i), part(x_in, i), 9, x_recv.at[i], away)

        def fold(i):
            zz, k, w, _ = units[i]
            remote(part(core_out, i), part(core_in, i), 0, core_recv.at[i], next_core).wait_recv()

            def pieces(lines):
                for j in range(w):
                    b = zz * np_ + k + j
                    yield b, keep[i % 3, lines, pl.ds(j * dc, dc)] + core_in[b, lines, :].astype(f32)

            def through_y():
                for b, amount in pieces(their_rows):
                    y_out[b] = amount.astype(bf)
                by_y(i).start()
                for j in range(w):
                    b, lanes = zz * np_ + k + j, pl.ds(j * dc, dc)
                    keep[i % 3, mine_rows, lanes] = (keep[i % 3, mine_rows, lanes]
                                                     + core_in[b, mine_rows, :].astype(f32))

            if not RAW[i]:
                through_y()
                return

            def put(lines):
                for b, amount in pieces(lines):
                    core_in[b, lines, :] = amount.astype(bf)

            @pl.when(core == 0)
            def _():
                through_y()

            @pl.when(core == 1)
            def _():
                if RAW[i] == 3:
                    for gg in range(2):
                        put(pl.ds(gg * rows, rows))
                        turn(i, gg).start()
                    return
                for own in range(2):
                    put(mine_rows if own else their_rows)
                    if RAW[i] == 2 and not own:
                        direct(i).start()
                    else:
                        raw_half(i, own, 10).start()

        def add(i):
            zz, k, w, _ = units[i]

            def through_x():
                by_y(i).wait_recv()
                for j in range(w):
                    b, lanes = zz * np_ + k + j, pl.ds(j * dc, dc)
                    xz_out[b] = (keep[i % 3, mine_rows, lanes] + y_in[b].astype(f32)).astype(bf)
                sent_away(i).start()

            if not RAW[i]:
                through_x()
                return

            @pl.when(core == 0)
            def _():
                through_x()

            if RAW[i] == 3:
                @pl.when(core == 1)
                def _():
                    took(part(y_in, i), y_recv.at[i])
                    for own in range(2):
                        gg = g if own else 1 - g
                        lines = at(gg, fold_rows)
                        kept = pl.ds(pl.multiple_of(gg * rows + x * fold_rows, fold_rows), fold_rows)
                        for j in range(w):
                            b = zz * np_ + k + j
                            xz_out[b, lines, :] = (core_in[b, kept, :].astype(f32)
                                                   + y_in[b, lines, :].astype(f32)).astype(bf)
                        remote(strip(xz_out, i, gg), strip(x_in, i, gg), 12, (raw_recv if own else core_recv).at[i],
                               {"fs": outer}).start()

        def finish(i):
            @pl.when(core == 0)
            def _():
                sent_away(i).wait_recv()
                value(i, xz_out, x_in)
                share(i).start()
                write(i)

        def ready(i):
            zz, k, w, j = units[i]
            if j > 1:
                took(down.at[pl.ds(zz * np_ + k, w)], slot(1, zz, 2 * k, j - 1)[1])

        for s in STEPS:
            i = int(s[1:])
            if s[0] == "P":
                if i == n - 1:
                    project_last(i)
                else:
                    ready(i)
                    project(i)
                if i < 2:
                    forward_down(i)
            else:
                {"F": fold, "A": add, "N": finish}[s[0]](i)
        gave(tok.at[pl.ds(0, 11 * quarter), :], 1)
        for s in (3, 4):
            gave(up.at[pl.ds(0, depth), :], s)
        for s in (5, 6):
            gave(down.at[pl.ds(0, np_)], s)
        gave(core_out, 7)

        @pl.when(core == 0)
        def _():
            gave(y_out, 8)
            gave(xz_out, 9)
            gave(branch, 2)

        @pl.when(core == 1)
        def _():
            gave(y_out.at[pl.ds(0, total(0))], 8)
            gave(xz_out.at[pl.ds(0, total(0))], 9)
            gave(core_in.at[pl.ds(0, total(1, 2))], 10)
            if total(3):
                gave(y_in.at[pl.ds(0, total(3))], 11)
                gave(xz_out.at[pl.ds(0, total(3))], 12)
            receive(range(n))

    gave(scl.at[pl.ds(0, 3)], 0)
    pltpu.make_async_copy(branch, out, one_sem.at[2]).wait()


def closing(branch, tokens, post_gain, out, rows_in, rows_out, arrive, bring, leave):
    parts = arrive.shape[0]
    step = tokens.shape[0] // parts

    def place(i):
        return pl.ds(pl.multiple_of(i * step, step), step)

    def fetch(i):
        return pltpu.make_async_copy(branch.at[:, place(i), :], rows_in.at[:, place(i), :], arrive.at[i])

    def residual(i):
        return pltpu.make_async_copy(tokens.at[place(i), :], rows_out.at[place(i), :], bring.at[i])

    for i in range(parts):
        fetch(i).start()
        residual(i).start()

    def one(i, _):
        fetch(i).wait()
        residual(i).wait()
        row = jnp.concatenate([rows_in[b, place(i), :] for b in range(branch.shape[0])], axis=1).astype(jnp.float32)
        rows_out[place(i), :] = (rows_out[place(i), :].astype(jnp.float32) + rms_rows(row, post_gain[...])).astype(jnp.bfloat16)
        pltpu.make_async_copy(rows_out.at[place(i), :], out.at[place(i), :], leave.at[0]).start()
        return 0

    lax.fori_loop(0, parts, one, 0)
    pltpu.make_async_copy(rows_out, out, leave.at[0]).wait()


def fused(tokens, pre_gain, up_weight, up_scale, down_weight, down_scale, post_gain):
    rows, width = tokens.shape
    depth, ff = up_weight.shape
    half, dc = ff // 2, depth // PIECES
    pieces = 4 * PIECES
    n = sum(len(w) for w in WIDTHS)
    bf, f32 = jnp.bfloat16, jnp.float32
    dma = pltpu.SemaphoreType.DMA
    anywhere, vmem = pl.BlockSpec(memory_space=pl.ANY), pl.BlockSpec(memory_space=pltpu.VMEM)
    branch = pl.pallas_call(
        kernel,
        out_shape=jax.ShapeDtypeStruct((pieces, rows, dc), bf),
        in_specs=[anywhere, anywhere, anywhere, vmem, vmem, vmem],
        out_specs=anywhere,
        scratch_shapes=[
            pltpu.VMEM((rows, width), bf),
            pltpu.VMEM((depth, half), f32),
            pltpu.VMEM((half, depth), f32),
            pltpu.VMEM((width, half), bf),
            pltpu.VMEM((pieces, half, dc), bf),
            pltpu.VMEM((4 * rows, width), bf),
            pltpu.VMEM((4 * rows, half), f32),
            pltpu.VMEM((4 * rows, half), bf),
            pltpu.VMEM((4, 1, depth), f32),
            pltpu.VMEM((3, 2 * rows, 2 * dc), f32),
            pltpu.VMEM((pieces, 2 * rows, dc), bf),
            pltpu.VMEM((pieces, 2 * rows, dc), bf),
            pltpu.VMEM((pieces, rows, dc), bf),
            pltpu.VMEM((pieces, rows, dc), bf),
            pltpu.VMEM((pieces, rows, dc), bf),
            pltpu.VMEM((pieces, rows, dc), bf),
            pltpu.VMEM((pieces, rows, dc), bf),
            dma((13,)),
            dma((6,)),
            dma((8,)),
            dma((4, PIECES)),
            dma((1,)),
            dma((n,)),
            dma((n,)),
            dma((n,)),
            dma((n,)),
            dma((n,)),
            dma((PIECES + 1,)),
            dma((3,)),
        ],
        compiler_params=pltpu.CompilerParams(
            collective_id=0, has_side_effects=True, vmem_limit_bytes=58 << 20
        ),
    )(tokens, up_weight, down_weight, up_scale.reshape(1, ff), down_scale.reshape(1, depth),
      pre_gain.reshape(1, width))
    parts = 8
    far = pl.BlockSpec(memory_space=pltpu.HBM)
    return pl.pallas_call(
        closing,
        out_shape=jax.ShapeDtypeStruct((rows, width), bf),
        in_specs=[far, far, vmem],
        out_specs=far,
        scratch_shapes=[pltpu.VMEM((pieces, rows, dc), bf), pltpu.VMEM((rows, width), bf), dma((parts,)), dma((parts,)), dma((1,))],
        compiler_params=pltpu.CompilerParams(vmem_limit_bytes=60 << 20),
    )(branch, tokens, post_gain.reshape(1, width))


def solution(mesh):
    placed = (P(("grp", "fs"), None), P(), P("fs", "tp"), P("tp"), P("tp", "fs"), P("fs"), P())
    sizes = mesh.shape
    line = sizes["grp"] == 2 and sizes["fs"] == 4 and sizes["tp"] == 4
    return jax.shard_map(
        fused if line else plain, mesh=mesh, in_specs=placed, out_specs=P(("grp", "fs"), None), check_vma=False
    )
```

```python
import jax
import jax.numpy as jnp
from jax import lax
from jax.experimental import pallas as pl
from jax.experimental.pallas import tpu as pltpu
from jax.sharding import PartitionSpec as P

epsilon = 1e-06
MESH = pl.DeviceIdType.MESH
PIECES = 4
WIDTHS = ((2, 2), (2, 2), (2, 2), (2, 1, 1))
RAW = (0, 1, 0, 1, 0, 1, 2, 2, 2)
ORDER = ("P0F0P1F1P2F2A0P3F3A1N0P4F4A2P5F5A3N1", "A4N2P6F6A5N3P7F7A6N4P8F8A7N5A8N6N7N8")
STEPS = tuple(part[i:i + 2] for part in ORDER for i in range(0, len(part), 2))
ARRIVAL = tuple(int(s[1:]) for s in STEPS if s[0] == "AFFA"[RAW[int(s[1:])]])


def rms_rows(values, scaling):
    return values * lax.rsqrt(jnp.mean(values * values, axis=-1, keepdims=True) + epsilon) * scaling


def activate(lifted, up_scale):
    return jnp.square(jax.nn.relu(lifted * up_scale)).astype(jnp.bfloat16)


def plain(tokens, pre_gain, up_weight, up_scale, down_weight, down_scale, post_gain):
    residual = tokens.astype(jnp.float32)
    normed = rms_rows(residual, pre_gain).astype(jnp.bfloat16)
    up_cast = up_weight.astype(jnp.bfloat16)
    down_cast = down_weight.astype(jnp.bfloat16)
    column_scales = lax.all_gather(down_scale, "fs", axis=0, tiled=True)
    up_full, down_full = (
        lax.all_gather(up_cast, "fs", axis=0, tiled=True),
        lax.all_gather(down_cast, "fs", axis=1, tiled=True),
    )
    lifted = jnp.dot(normed, up_full, preferred_element_type=jnp.float32)
    hidden = activate(lifted, up_scale)
    partials = jnp.dot(hidden, down_full, preferred_element_type=jnp.float32)
    partials = (partials * column_scales).astype(jnp.bfloat16)
    summed = lax.psum(partials, "tp").astype(jnp.float32)
    branch = lax.optimization_barrier(summed.astype(jnp.bfloat16)).astype(jnp.float32)
    return (residual + rms_rows(branch, post_gain)).astype(jnp.bfloat16)


def kernel(tokens, up_in, down_in, up_scale, down_scale, pre_gain, out, res, up_f32, down_f32, up, down,
           tok, acc, hid, scl, keep, core_out, core_in, y_out, y_in, xz_out, x_in, branch, send, up_recv, down_recv,
           tok_recv, scl_recv, core_recv, y_recv, x_recv, raw_recv, br_recv,
           local, one_sem):
    g, z, t = lax.axis_index("grp"), lax.axis_index("fs"), lax.axis_index("tp")
    core, x = lax.rem(t, 2), t // 2
    pair = z // 2
    outer, inner, other = 3 * pair, 1 + pair, 2 - pair
    outer2 = 3 - outer
    is_outer = z == outer
    n_tp, np_ = 4, PIECES
    rows, width = tokens.shape
    depth, half = up_in.shape[0], up_in.shape[1] // 2
    du, dc, quarter = depth // np_, depth // np_, rows // np_
    core_peer, x_peer, cross_peer = x * 2 + 1 - core, (1 - x) * 2 + core, (1 - x) * 2 + 1 - core
    bf, f32 = jnp.bfloat16, jnp.float32

    def at(i, size):
        return pl.ds(pl.multiple_of(i * size, size), size)

    def load(kind, c):
        if kind == 0:
            copy = up_in.at[pl.ds(c * du, du), at(g, half)], up_f32.at[pl.ds(c * du, du), :]
        else:
            copy = down_in.at[at(g, half), :], down_f32
        return pltpu.make_async_copy(*copy, local.at[np_ if kind else c])

    load(0, 0).start()
    fetch = pltpu.make_async_copy(tokens, res, one_sem.at[0])
    fetch.start()
    for c in range(1, np_):
        load(0, c).start()
    load(1, 0).start()

    barrier = pltpu.get_barrier_semaphore()
    peers = [{"fs": lax.rem(z + o, 4)} for o in range(1, 4)] + [{"grp": 1 - g}]
    peers += [{"tp": lax.rem(t + o, n_tp)} for o in range(1, n_tp)]
    peers += [{"grp": 1 - g, "fs": z + 1 - 2 * lax.rem(z, 2)}]
    for peer in peers:
        pl.semaphore_signal(barrier, inc=1, device_id=peer, device_id_type=MESH)
    pl.semaphore_wait(barrier, len(peers))

    def remote(src, dst, s, r, peer):
        return pltpu.make_async_remote_copy(src_ref=src, dst_ref=dst, send_sem=send.at[s], recv_sem=r,
                                            device_id=peer, device_id_type=MESH)

    def same(ref, s, r, peer):
        return remote(ref, ref, s, r, peer)

    def slot(kind, zz, c, stage):
        if kind == 0:
            return up.at[at(zz * np_ + c, du), :], up_recv.at[c if stage == 0 else 3 + stage]
        mark = 2 * stage + c // 4 if stage < 2 or c < 4 else 5 + max(0, c - 5)
        return down.at[zz * np_ + c // 2, pl.ds(c % 2 * (half // 2), half // 2), :], down_recv.at[mark]

    def cast(kind, c):
        if kind == 0 or c == 0:
            load(kind, c).wait()
        if kind == 0:
            up[at(z * np_ + c, du), :] = up_f32[pl.ds(c * du, du), :].astype(bf)
        else:
            down[z * np_ + c] = down_f32[:, pl.ds(c * dc, dc)].astype(bf)

    def weight(kind, zz, c, stage, s, peer):
        ref, r = slot(kind, zz, c, stage)
        same(ref, s, r, peer).start()

    def took(ref, r):
        same(ref, 0, r, {"fs": other}).wait_recv()

    def gave(ref, s):
        same(ref, s, scl_recv.at[0], {"fs": other}).wait_send()

    def piece(gg, kind, k):
        b = kind * 2 + gg
        return tok.at[at(b * np_ + k, quarter), :], tok_recv.at[b, k]

    def pass_tok(gg, kind, k, peer):
        ref, r = piece(gg, kind, k)
        same(ref, 1, r, peer).start()

    def have_tok(gg, kind, k):
        took(*piece(gg, kind, k))

    def norm(b, k):
        def one(i, _):
            source = pl.ds(pl.multiple_of(k * quarter + i * 64, 64), 64)
            target = pl.ds(pl.multiple_of((b * np_ + k) * quarter + i * 64, 64), 64)
            tok[target, :] = rms_rows(res[source, :].astype(f32), pre_gain[...]).astype(bf)
            return 0
        lax.fori_loop(0, quarter // 64, one, 0)

    blocks = (inner, outer, other, outer2)
    units = []
    for j, widths in enumerate(WIDTHS):
        k = 0
        for w in widths:
            units.append((blocks[j], k, w, j))
            k += w
    n = len(units)

    def total(*modes):
        return sum(u[2] for u, raw in zip(units, RAW) if raw in modes)

    def part(ref, i):
        zz, k, w, _ = units[i]
        return ref.at[pl.ds(zz * np_ + k, w)]

    mine_rows, their_rows = at(g, rows), at(1 - g, rows)

    def half_of(ref, i, lines):
        zz, k, w, _ = units[i]
        return ref.at[pl.ds(zz * np_ + k, w), lines, :]

    fold_rows = rows // 2

    def strip(ref, i, gg):
        return half_of(ref, i, at(gg, fold_rows))

    def raw_half(i, own, s):
        lines = mine_rows if own else their_rows
        ref = half_of(core_in, i, lines)
        return same(ref, s, (raw_recv if own else core_recv).at[i], {"fs": outer})

    def value(i, first, second):
        zz, k, w, _ = units[i]
        for j in range(w):
            b = zz * np_ + k + j
            total = first[b].astype(f32) + second[b].astype(f32)
            branch[b] = (total * scl[zz, :, pl.ds((k + j) * dc, dc)]).astype(bf)

    def write(i):
        pltpu.make_async_copy(part(branch, i), part(out, i), one_sem.at[2]).start()

    def receive(order):
        for i in order:
            took(part(branch, i), br_recv.at[i])
            write(i)

    def share(i):
        return same(part(branch, i), 2, br_recv.at[i], {"tp": core_peer})

    for o in range(1, 4):
        remote(down_scale, scl.at[z], 0, scl_recv.at[0], {"fs": lax.rem(z + o, 4)}).start()
    own_scale = pltpu.make_async_copy(down_scale, scl.at[z], one_sem.at[1])
    own_scale.start()

    def scales():
        own_scale.wait()
        took(scl.at[pl.ds(0, 3)], scl_recv.at[0])

    @pl.when(is_outer)
    def _():
        to = {"fs": inner}
        fetch.wait()
        norm(2 + g, t)
        pass_tok(g, 1, t, to)
        for c in range(np_):
            cast(0, c)
            weight(0, z, c, 0, 3, to)
        for c in range(np_):
            cast(1, c)
            for k in range(2):
                weight(1, z, 2 * c + k, 0, 4, to)
        scales()

        @pl.when(core == 1)
        def _():
            def relay(i):
                return remote(part(x_in, i), part(y_in, i), 5, y_recv.at[i], {"tp": x_peer})

            def side(i):
                return remote(half_of(core_in, i, their_rows), part(y_in, i), 6, y_recv.at[i], {"grp": 1 - g})

            def swap(i):
                return remote(part(xz_out, i), part(x_in, i), 7, x_recv.at[i], {"tp": x_peer})

            def side_strip(i):
                return remote(strip(x_in, i, 1 - g), strip(y_in, i, 0), 9, y_recv.at[i], {"grp": 1 - g})

            def swap_strip(i, xx):
                return same(strip(branch, i, xx), 8, x_recv.at[i], {"tp": x_peer})

            def first(i):
                if RAW[i] == 3:
                    took(strip(x_in, i, 1 - g), core_recv.at[i])
                    side_strip(i).start()
                elif RAW[i] == 2:
                    raw_half(i, True, 0).wait_recv()
                elif RAW[i]:
                    raw_half(i, False, 0).wait_recv()
                    side(i).start()
                else:
                    remote(part(x_in, i), part(x_in, i), 0, x_recv.at[i], {"fs": inner}).wait_recv()
                    relay(i).start()

            def second(i):
                zz, k, w, _ = units[i]
                if RAW[i] == 3:
                    took(strip(x_in, i, g), raw_recv.at[i])
                    side_strip(i).wait_recv()
                    for j in range(w):
                        b = zz * np_ + k + j
                        both = x_in[b, at(g, fold_rows), :].astype(f32) + y_in[b, pl.ds(0, fold_rows), :].astype(f32)
                        branch[b, at(x, fold_rows), :] = (both * scl[zz, :, pl.ds((k + j) * dc, dc)]).astype(bf)
                    swap_strip(i, x).start()
                    return
                if RAW[i] == 1:
                    raw_half(i, True, 0).wait_recv()
                side(i).wait_recv()
                for j in range(w):
                    b = zz * np_ + k + j
                    xz_out[b] = (core_in[b, mine_rows, :].astype(f32) + y_in[b].astype(f32)).astype(bf)
                swap(i).start()

            def third(i):
                if RAW[i] == 3:
                    swap_strip(i, 1 - x).wait_recv()
                elif RAW[i]:
                    swap(i).wait_recv()
                    value(i, xz_out, x_in)
                else:
                    relay(i).wait_recv()
                    value(i, x_in, y_in)
                share(i).start()
                write(i)

            for s in range(n + 2):
                if s < n:
                    first(ARRIVAL[s])
                if 0 <= s - 1 < n:
                    i = ARRIVAL[s - 1]
                    if RAW[i]:
                        second(i)
                    else:
                        third(i)
                if 0 <= s - 2 < n and RAW[ARRIVAL[s - 2]]:
                    third(ARRIVAL[s - 2])
            gave(x_in.at[pl.ds(0, total(0))], 5)
            if total(1):
                gave(x_in.at[pl.ds(0, total(1))], 6)
            if total(3):
                for s in (8, 9):
                    gave(x_in.at[pl.ds(0, total(3)), pl.ds(0, fold_rows), :], s)
            gave(x_in.at[pl.ds(0, total(1, 2))], 7)
            gave(branch, 2)

        @pl.when(core == 0)
        def _():
            receive(ARRIVAL)

        gave(tok.at[pl.ds(0, quarter), :], 1)
        gave(up.at[pl.ds(0, depth), :], 3)
        gave(down.at[pl.ds(0, np_)], 4)

    @pl.when(jnp.logical_not(is_outer))
    def _():
        across, beside, next_core = {"fs": other}, {"grp": 1 - g}, {"tp": core_peer}
        for c in range(np_):
            cast(0, c)
            weight(0, z, c, 1, 3, across)
        fetch.wait()
        for j in range(np_):
            k = lax.rem(core * 2 + j, 4)
            norm(g, k)
            if j < 2:
                pass_tok(g, 0, k, beside)
        for c in range(np_):
            cast(1, c)

        have_tok(g, 1, t)
        for peer in ({"tp": x_peer}, beside, next_core, {"tp": cross_peer}):
            pass_tok(g, 1, t, peer)

        def forward(c):
            took(*slot(0, outer, c, 0))
            weight(0, outer, c, 2, 4, across)

        def forward_down(c):
            took(down.at[pl.ds(outer * np_ + 2 * c, 2)], down_recv.at[c])
            for k in range(4):
                weight(1, outer, 4 * c + k, 2, 6, across)

        def hand_on(kind, k):
            have_tok(1 - g, kind, k)
            pass_tok(1 - g, kind, k, next_core)

        forward(0)
        hand_on(0, core * 2)
        forward(1)
        hand_on(0, core * 2 + 1)
        have_tok(g, 1, x_peer)
        pass_tok(g, 1, x_peer, beside)
        forward(2)
        forward(3)
        for c in range(2 * np_):
            weight(1, z, c, 1, 5, across)

        tile = 512
        most = 3 * depth
        low, rest = pair * depth, outer2 * depth
        most_at = pl.ds(pl.multiple_of(low, depth), most)
        rest_at = pl.ds(pl.multiple_of(rest, depth), depth)

        def lift_most(b):
            lines = at(b, rows)

            def one(i, _):
                columns = at(i, tile)
                acc[lines, columns] = jnp.dot(tok[lines, most_at], up[most_at, columns], preferred_element_type=f32)
                return 0
            lax.fori_loop(0, half // tile, one, 0)

        def lift_all(b):
            lines = at(b, rows)

            def one(i, _):
                columns = at(i, tile)
                lifted = jnp.dot(tok[lines, :], up[:, columns], preferred_element_type=f32)
                whole = pl.ds(pl.multiple_of(g * half + i * tile, tile), tile)
                hid[lines, columns] = activate(lifted, up_scale[:, whole])
                return 0
            lax.fori_loop(0, half // tile, one, 0)

        def lift_rest(b):
            lines = at(b, rows)

            def one(i, _):
                columns = at(i, tile)
                lifted = acc[lines, columns] + jnp.dot(tok[lines, rest_at], up[rest_at, columns],
                                                       preferred_element_type=f32)
                whole = pl.ds(pl.multiple_of(g * half + i * tile, tile), tile)
                hid[lines, columns] = activate(lifted, up_scale[:, whole])
                return 0
            lax.fori_loop(0, half // tile, one, 0)

        took(up.at[at(other, depth), :], up_recv.at[4])
        lift_most(g)
        have_tok(g, 1, core_peer)
        have_tok(g, 1, cross_peer)
        lift_most(2 + g)
        hand_on(1, t)
        have_tok(1 - g, 0, lax.rem(core * 2 + 2, 4))
        have_tok(1 - g, 0, lax.rem(core * 2 + 3, 4))
        lift_most(1 - g)
        hand_on(1, x_peer)
        took(up.at[at(outer2, depth), :], up_recv.at[5])
        for b in (g, 2 + g, 1 - g):
            lift_rest(b)
        have_tok(1 - g, 1, core_peer)
        have_tok(1 - g, 1, cross_peer)
        lift_all(3 - g)
        scales()

        mine, theirs = at(core, 2 * rows), at(1 - core, 2 * rows)
        def project(i):
            zz, k, w, _ = units[i]
            b = zz * np_ + k
            weights = down[b] if w == 1 else jnp.concatenate([down[b + j] for j in range(w)], axis=1)
            product = jnp.dot(hid[theirs, :], weights, preferred_element_type=f32).astype(bf)
            for j in range(w):
                core_out[b + j] = product[:, j * dc:(j + 1) * dc]
            keep[i % 3, :, pl.ds(0, w * dc)] = jnp.dot(hid[mine, :], weights, preferred_element_type=f32)
            remote(part(core_out, i), part(core_in, i), 7, core_recv.at[i], next_core).start()

        def project_last(i):
            zz, k, _, _ = units[i]
            b = zz * np_ + k
            early, late = pl.ds(0, half // 2), pl.ds(half // 2, half // 2)
            lanes = pl.ds(0, dc)
            took(*slot(1, zz, 2 * k, 2))
            acc[pl.ds(0, 2 * rows), lanes] = jnp.dot(hid[theirs, early], down[b, early, :], preferred_element_type=f32)
            keep[i % 3, :, lanes] = jnp.dot(hid[mine, early], down[b, early, :], preferred_element_type=f32)
            took(*slot(1, zz, 2 * k + 1, 2))
            core_out[b] = (acc[pl.ds(0, 2 * rows), lanes] + jnp.dot(
                hid[theirs, late], down[b, late, :], preferred_element_type=f32)).astype(bf)
            keep[i % 3, :, lanes] = keep[i % 3, :, lanes] + jnp.dot(
                hid[mine, late], down[b, late, :], preferred_element_type=f32)
            remote(part(core_out, i), part(core_in, i), 7, core_recv.at[i], next_core).start()

        away = {"fs": jnp.where(core == 0, z, outer), "tp": jnp.where(core == 0, x_peer, t)}

        def by_y(i):
            return remote(part(y_out, i), part(y_in, i), 8, y_recv.at[i], beside)

        def turn(i, gg):
            lines = pl.ds(pl.multiple_of(gg * rows + (1 - x) * fold_rows, fold_rows), fold_rows)
            return remote(half_of(core_in, i, lines), strip(y_in, i, gg), 11, y_recv.at[i], {"tp": x_peer})

        def direct(i):
            return remote(half_of(core_in, i, their_rows), part(y_in, i), 10, y_recv.at[i],
                          {"grp": 1 - g, "fs": outer})

        def sent_away(i):
            return remote(part(xz_out, i), part(x_in, i), 9, x_recv.at[i], away)

        def fold(i):
            zz, k, w, _ = units[i]
            remote(part(core_out, i), part(core_in, i), 0, core_recv.at[i], next_core).wait_recv()

            def pieces(lines):
                for j in range(w):
                    b = zz * np_ + k + j
                    yield b, keep[i % 3, lines, pl.ds(j * dc, dc)] + core_in[b, lines, :].astype(f32)

            def through_y():
                for b, amount in pieces(their_rows):
                    y_out[b] = amount.astype(bf)
                by_y(i).start()
                for j in range(w):
                    b, lanes = zz * np_ + k + j, pl.ds(j * dc, dc)
                    keep[i % 3, mine_rows, lanes] = (keep[i % 3, mine_rows, lanes]
                                                     + core_in[b, mine_rows, :].astype(f32))

            if not RAW[i]:
                through_y()
                return

            def put(lines):
                for b, amount in pieces(lines):
                    core_in[b, lines, :] = amount.astype(bf)

            @pl.when(core == 0)
            def _():
                through_y()

            @pl.when(core == 1)
            def _():
                if RAW[i] == 3:
                    for gg in range(2):
                        put(pl.ds(gg * rows, rows))
                        turn(i, gg).start()
                    return
                for own in range(2):
                    put(mine_rows if own else their_rows)
                    if RAW[i] == 2 and not own:
                        direct(i).start()
                    else:
                        raw_half(i, own, 10).start()

        def add(i):
            zz, k, w, _ = units[i]

            def through_x():
                by_y(i).wait_recv()
                for j in range(w):
                    b, lanes = zz * np_ + k + j, pl.ds(j * dc, dc)
                    xz_out[b] = (keep[i % 3, mine_rows, lanes] + y_in[b].astype(f32)).astype(bf)
                sent_away(i).start()

            if not RAW[i]:
                through_x()
                return

            @pl.when(core == 0)
            def _():
                through_x()

            if RAW[i] == 3:
                @pl.when(core == 1)
                def _():
                    took(part(y_in, i), y_recv.at[i])
                    for own in range(2):
                        gg = g if own else 1 - g
                        lines = at(gg, fold_rows)
                        kept = pl.ds(pl.multiple_of(gg * rows + x * fold_rows, fold_rows), fold_rows)
                        for j in range(w):
                            b = zz * np_ + k + j
                            xz_out[b, lines, :] = (core_in[b, kept, :].astype(f32)
                                                   + y_in[b, lines, :].astype(f32)).astype(bf)
                        remote(strip(xz_out, i, gg), strip(x_in, i, gg), 12, (raw_recv if own else core_recv).at[i],
                               {"fs": outer}).start()

        def finish(i):
            @pl.when(core == 0)
            def _():
                sent_away(i).wait_recv()
                value(i, xz_out, x_in)
                share(i).start()
                write(i)

        def ready(i):
            zz, k, w, j = units[i]
            if j > 1:
                took(down.at[pl.ds(zz * np_ + k, w)], slot(1, zz, 2 * k, j - 1)[1])

        for s in STEPS:
            i = int(s[1:])
            if s[0] == "P":
                if i == n - 1:
                    project_last(i)
                else:
                    ready(i)
                    project(i)
                if i < 2:
                    forward_down(i)
            else:
                {"F": fold, "A": add, "N": finish}[s[0]](i)
        gave(tok.at[pl.ds(0, 11 * quarter), :], 1)
        for s in (3, 4):
            gave(up.at[pl.ds(0, depth), :], s)
        for s in (5, 6):
            gave(down.at[pl.ds(0, np_)], s)
        gave(core_out, 7)

        @pl.when(core == 0)
        def _():
            gave(y_out, 8)
            gave(xz_out, 9)
            gave(branch, 2)

        @pl.when(core == 1)
        def _():
            gave(y_out.at[pl.ds(0, total(0))], 8)
            gave(xz_out.at[pl.ds(0, total(0))], 9)
            gave(core_in.at[pl.ds(0, total(1, 2))], 10)
            if total(3):
                gave(y_in.at[pl.ds(0, total(3))], 11)
                gave(xz_out.at[pl.ds(0, total(3))], 12)
            receive(range(n))

    gave(scl.at[pl.ds(0, 3)], 0)
    pltpu.make_async_copy(branch, out, one_sem.at[2]).wait()


def closing(branch, tokens, post_gain, out, rows_in, rows_out, arrive, bring, leave):
    parts = arrive.shape[0]
    step = tokens.shape[0] // parts

    def place(i):
        return pl.ds(pl.multiple_of(i * step, step), step)

    def fetch(i):
        return pltpu.make_async_copy(branch.at[:, place(i), :], rows_in.at[:, place(i), :], arrive.at[i])

    def residual(i):
        return pltpu.make_async_copy(tokens.at[place(i), :], rows_out.at[place(i), :], bring.at[i])

    for i in range(parts):
        fetch(i).start()
        residual(i).start()

    def one(i, _):
        fetch(i).wait()
        residual(i).wait()
        row = jnp.concatenate([rows_in[b, place(i), :] for b in range(branch.shape[0])], axis=1).astype(jnp.float32)
        rows_out[place(i), :] = (rows_out[place(i), :].astype(jnp.float32) + rms_rows(row, post_gain[...])).astype(jnp.bfloat16)
        pltpu.make_async_copy(rows_out.at[place(i), :], out.at[place(i), :], leave.at[0]).start()
        return 0

    lax.fori_loop(0, parts, one, 0)
    pltpu.make_async_copy(rows_out, out, leave.at[0]).wait()


def fused(tokens, pre_gain, up_weight, up_scale, down_weight, down_scale, post_gain):
    rows, width = tokens.shape
    depth, ff = up_weight.shape
    half, dc = ff // 2, depth // PIECES
    pieces = 4 * PIECES
    n = sum(len(w) for w in WIDTHS)
    bf, f32 = jnp.bfloat16, jnp.float32
    dma = pltpu.SemaphoreType.DMA
    anywhere, vmem = pl.BlockSpec(memory_space=pl.ANY), pl.BlockSpec(memory_space=pltpu.VMEM)
    branch = pl.pallas_call(
        kernel,
        out_shape=jax.ShapeDtypeStruct((pieces, rows, dc), bf),
        in_specs=[anywhere, anywhere, anywhere, vmem, vmem, vmem],
        out_specs=anywhere,
        scratch_shapes=[
            pltpu.VMEM((rows, width), bf),
            pltpu.VMEM((depth, half), f32),
            pltpu.VMEM((half, depth), f32),
            pltpu.VMEM((width, half), bf),
            pltpu.VMEM((pieces, half, dc), bf),
            pltpu.VMEM((4 * rows, width), bf),
            pltpu.VMEM((4 * rows, half), f32),
            pltpu.VMEM((4 * rows, half), bf),
            pltpu.VMEM((4, 1, depth), f32),
            pltpu.VMEM((3, 2 * rows, 2 * dc), f32),
            pltpu.VMEM((pieces, 2 * rows, dc), bf),
            pltpu.VMEM((pieces, 2 * rows, dc), bf),
            pltpu.VMEM((pieces, rows, dc), bf),
            pltpu.VMEM((pieces, rows, dc), bf),
            pltpu.VMEM((pieces, rows, dc), bf),
            pltpu.VMEM((pieces, rows, dc), bf),
            pltpu.VMEM((pieces, rows, dc), bf),
            dma((13,)),
            dma((6,)),
            dma((8,)),
            dma((4, PIECES)),
            dma((1,)),
            dma((n,)),
            dma((n,)),
            dma((n,)),
            dma((n,)),
            dma((n,)),
            dma((PIECES + 1,)),
            dma((3,)),
        ],
        compiler_params=pltpu.CompilerParams(
            collective_id=0, has_side_effects=True, vmem_limit_bytes=58 << 20
        ),
    )(tokens, up_weight, down_weight, up_scale.reshape(1, ff), down_scale.reshape(1, depth),
      pre_gain.reshape(1, width))
    parts = 8
    far = pl.BlockSpec(memory_space=pltpu.HBM)
    return pl.pallas_call(
        closing,
        out_shape=jax.ShapeDtypeStruct((rows, width), bf),
        in_specs=[far, far, vmem],
        out_specs=far,
        scratch_shapes=[pltpu.VMEM((pieces, rows, dc), bf), pltpu.VMEM((rows, width), bf), dma((parts,)), dma((parts,)), dma((1,))],
        compiler_params=pltpu.CompilerParams(vmem_limit_bytes=60 << 20),
    )(branch, tokens, post_gain.reshape(1, width))


def solution(mesh):
    placed = (P(("grp", "fs"), None), P(), P("fs", "tp"), P("tp"), P("tp", "fs"), P("fs"), P())
    sizes = mesh.shape
    line = sizes["grp"] == 2 and sizes["fs"] == 4 and sizes["tp"] == 4
    return jax.shard_map(
        fused if line else plain, mesh=mesh, in_specs=placed, out_specs=P(("grp", "fs"), None), check_vma=False
    )
```
